32 devices in a mesh: sp: 16 (over z, y, x), dp: 2 (over core).
Axes of the slice: x: 2, y: 2, z: 4, core: 2. Of those that a mesh axis runs over, the one named last changes fastest.
Arguments:
- inputs: bfloat16 [2, 2048, 2048], P('dp', 'sp'), may hold values from -6 to 6
- conv_weight: bfloat16 [4, 2048], replicated, may hold values from -3 to 3
- gate_weight: bfloat16 [2, 8, 256, 256], P(None, 'dp'), may hold values from -0.375 to 0.375
- rate_param: float32 [2048], replicated, may hold values from 4 to 12.5
- pace: float32 [2, 2048], P('dp'), may hold values from 0.5 to 30000
Outputs:
- recurrent: bfloat16 [2, 2048, 2048], P('dp', 'sp')
The draws below stay inside these ranges and needn't reach their ends.
All inputs are finite; a program needn't handle non-finite values.
Results may differ from the reference program's by a relative error of at most 0.008.
Values may be sent and summed in bfloat16 or wider, within the bound.
A program may use at most 128 MiB of HBM per device.

```python
import math
import jax
import jax.numpy as jnp
from jax import lax

TOK_DEV = 128
HEADS = 8
BLOCK = 256
CONV = 4
DR = 2048
SEQUENCE_COUNT = 2
SEQUENCE_LENGTH = 2048


def draw_rate_param(key, part):
    slow_share = 0.5
    slow_mask = jax.random.uniform(jax.random.fold_in(key, 21), (HEADS * BLOCK,), jnp.float32) < slow_share
    slow_value = jax.random.uniform(jax.random.fold_in(key, 22), (HEADS * BLOCK,), jnp.float32, 11.5, 12.5)
    fast_value = jax.random.uniform(jax.random.fold_in(key, 23), (HEADS * BLOCK,), jnp.float32, 4.0, 6.0)
    return jnp.where(slow_mask, slow_value, fast_value)


def draw_pace(key, part):
    block_count = SEQUENCE_LENGTH // TOK_DEV
    factor = jnp.exp(jax.random.uniform(jax.random.fold_in(key, 11), (SEQUENCE_COUNT, block_count), jnp.float32, math.log(0.5), math.log(2.0)))
    constant_level = jnp.repeat(factor, TOK_DEV, axis=1)
    surge_position = jax.random.randint(jax.random.fold_in(key, 12), (SEQUENCE_COUNT, 3), 0, SEQUENCE_LENGTH)
    surge_length = jax.random.uniform(jax.random.fold_in(key, 13), (SEQUENCE_COUNT, 3), jnp.float32, 6000.0, 10000.0)
    position_flags = jnp.arange(SEQUENCE_LENGTH, dtype=jnp.int32)[None, None, :] == surge_position[:, :, None]
    surge_spans = jnp.sum(jnp.where(position_flags, surge_length[:, :, None], 0.0), axis=1)
    return constant_level + surge_spans


def shard_levels(own_key, dims, split, least, largest):
    def one(axis_at, shards_of):
        draws = jax.random.uniform(jax.random.fold_in(jax.random.fold_in(own_key, 6), axis_at), (shards_of,), jnp.float32, least / len(split), largest / len(split))
        return jnp.repeat(jnp.exp(draws), dims[axis_at] // shards_of).reshape((-1,) + (1,) * (len(dims) - axis_at - 1))

    factor_of = one(*split[0])
    for cut in split[1:]:
        factor_of = factor_of * one(*cut)
    return factor_of


def bell_draw(stream_key, shape, scale, most, split=(), kind=jnp.bfloat16):
    values = jax.random.normal(stream_key, shape, jnp.float32) * scale
    if len(split) > 0:
        values = shard_levels(stream_key, shape, split, -0.22, 0.18) * values
    return jnp.clip(values, min=-most, max=most).astype(kind)


def setup_inputs(seed: int = 0) -> dict:
    keys = jax.random.split(jax.random.key(seed), 6)
    inputs = bell_draw(keys[0], (SEQUENCE_COUNT, SEQUENCE_LENGTH, DR), 1.0, 6.0, ((0, 2), (1, 16)))
    conv_weight = bell_draw(keys[1], (CONV, DR), CONV ** -0.5, 3.0)
    gate_weight = bell_draw(keys[2], (2, HEADS, BLOCK, BLOCK), BLOCK ** -0.5, 0.375, ((1, 2),))
    rate_param = draw_rate_param(jax.random.fold_in(keys[5], 71), 0)
    pace = draw_pace(jax.random.fold_in(keys[5], 71), 0)
    return {"inputs": inputs, "conv_weight": conv_weight, "gate_weight": gate_weight, "rate_param": rate_param, "pace": pace}


gate_power = 8.0

def combine(earlier, later):
    decay_e, state_e = earlier
    decay_l, state_l = later
    return (decay_e * decay_l, decay_l * state_e + state_l)

def lru_terms(pre_recur, pre_input, values, rate_col, pace_col):
    recur_gate = jax.nn.sigmoid(pre_recur.astype(jnp.float32))
    input_gate = jax.nn.sigmoid(pre_input.astype(jnp.float32))
    log_decay = -gate_power * pace_col * recur_gate * jax.nn.softplus(-rate_col)
    decay = jnp.exp(log_decay)
    drive = jnp.sqrt(-jnp.expm1(2.0 * log_decay)) * input_gate * values.astype(jnp.float32)
    return (decay, drive)

def reference(inputs, conv_weight, gate_weight, rate_param, pace):

    def one_sequence(pair):
        seq_rows, seq_pace = pair
        length = seq_rows.shape[0]
        padded = jnp.pad(seq_rows.astype(jnp.float32), ((CONV - 1, 0), (0, 0)))
        conv_taps = conv_weight.astype(jnp.float32)
        conv_out = jnp.zeros((length, seq_rows.shape[1]), jnp.float32)
        for tap in range(CONV):
            conv_out = conv_out + conv_taps[tap][None, :] * padded[tap:tap + length]
        conv_out = conv_out.astype(jnp.bfloat16)
        by_head = conv_out.reshape(length, HEADS, BLOCK).transpose(1, 0, 2)
        head_weights = gate_weight.transpose(1, 0, 2, 3)
        head_rates = rate_param.reshape(HEADS, BLOCK)

        def one_head(triple):
            head_rows, weights, rates = triple
            preact = jnp.einsum('ti,gij->gtj', head_rows.astype(jnp.float32), weights.astype(jnp.float32)).astype(jnp.bfloat16)
            decay, drive = lru_terms(preact[0], preact[1], head_rows, rates[None, :], seq_pace[:, None])
            _, state = lax.associative_scan(combine, (decay, drive), axis=0)
            return state.astype(jnp.bfloat16)
        states = lax.map(one_head, (by_head, head_weights, head_rates))
        return states.transpose(1, 0, 2).reshape(length, HEADS * BLOCK)
    return lax.map(one_sequence, (inputs, pace))
```

```python
import functools
import math

import jax
import jax.numpy as jnp
from jax import lax
from jax.experimental import pallas as pl
from jax.experimental.pallas import tpu as pltpu
from jax.sharding import PartitionSpec as P

CONV = 4
gate_power = 8.0
SUB = 8
LANES = 128
PIECE = SUB * LANES
TINY = 1.2e-38
LN2 = math.log(2.0)
SMALL = 0.07
MESH = pl.DeviceIdType.MESH


def softplus_neg(rate):
    e = jnp.exp(-jnp.abs(rate))
    series = e * (1.0 + e * (-0.5 + e * (1.0 / 3.0 + e * (-0.25 + e * 0.2))))
    return jnp.maximum(-rate, 0.0) + jnp.where(e < 0.03, series, jnp.log(1.0 + e))


def kernel(
    nsp, ndp, heads, block,
    x_hbm, cw_hbm, w_hbm, rate_hbm, pace_hbm, out_ref,
    x, cw, w, rate, pace_row, pace_mat, pace_perm, halo,
    hloc, acum, ex_h, ex_a, stage, send_buf, recv_buf, carry,
    load_sem, w_send, w_recv, halo_send, halo_recv, c_send, c_recv,
):
    me = lax.axis_index("sp")
    d = lax.axis_index("dp")
    count, width = x.shape
    steps = count // SUB
    hl = heads // ndp
    pieces = width // PIECE
    per = PIECE // block
    tiles = block // LANES

    barrier = pltpu.get_barrier_semaphore()

    @pl.loop(1, nsp)
    def _(o):
        pl.semaphore_signal(barrier, inc=1, device_id={"sp": lax.rem(me + o, nsp)}, device_id_type=MESH)

    @pl.loop(1, ndp)
    def _(o):
        pl.semaphore_signal(barrier, inc=1, device_id={"dp": lax.rem(d + o, ndp)}, device_id_type=MESH)

    first = pl.multiple_of(me * count, count)
    loads = [
        pltpu.make_async_copy(x_hbm.at[0], x, load_sem.at[0]),
        pltpu.make_async_copy(w_hbm, w.at[:, pl.ds(0, hl)], load_sem.at[1]),
        pltpu.make_async_copy(cw_hbm, cw, load_sem.at[2]),
        pltpu.make_async_copy(rate_hbm, rate, load_sem.at[3]),
        pltpu.make_async_copy(pace_hbm.at[:, pl.ds(first, count)], pace_row, load_sem.at[4]),
    ]
    for load in loads:
        load.start()

    @pl.when(me == 0)
    def _():
        halo[...] = jnp.zeros_like(halo)

    pl.semaphore_wait(barrier, nsp - 1 + ndp - 1)

    w_copies = []
    for o in range(1, ndp):
        w_copies.append(pltpu.make_async_remote_copy(
            src_ref=w_hbm,
            dst_ref=w.at[:, pl.ds(o * hl, hl)],
            send_sem=w_send.at[o],
            recv_sem=w_recv.at[o],
            device_id={"dp": lax.rem(d - o + ndp, ndp)},
            device_id_type=MESH,
        ))
    loads[0].wait()
    halo_copy = pltpu.make_async_remote_copy(
        src_ref=x.at[pl.ds(count - SUB, SUB)],
        dst_ref=halo,
        send_sem=halo_send.at[0],
        recv_sem=halo_recv.at[0],
        device_id={"sp": lax.rem(me + 1, nsp)},
        device_id_type=MESH,
    )

    @pl.when(me < nsp - 1)
    def _():
        halo_copy.start()

    for copy in w_copies:
        copy.start()
    for load in loads[1:]:
        load.wait()

    spread = jnp.broadcast_to(pace_row[...], (LANES, count)).T
    pace_mat[...] = spread
    for j in range(steps):
        pace_perm[j] = pace_mat[pl.ds(j, SUB, stride=steps), :]

    row = lax.broadcasted_iota(jnp.int32, (count, count), 0)
    col = lax.broadcasted_iota(jnp.int32, (count, count), 1)
    gather = jnp.where(col == (row % SUB) * steps + row // SUB, 1.0, 0.0).astype(jnp.bfloat16)
    scatter = jnp.where(row == (col % SUB) * steps + col // SUB, 1.0, 0.0).astype(jnp.bfloat16)
    sub = lax.broadcasted_iota(jnp.int32, (SUB, block), 0)

    @pl.when(me > 0)
    def _():
        halo_copy.wait_recv()

    def carry_copy(piece, src, dst):
        return pltpu.make_async_remote_copy(
            src_ref=send_buf.at[piece],
            dst_ref=recv_buf.at[src, piece],
            send_sem=c_send.at[dst, piece],
            recv_sem=c_recv.at[src, piece],
            device_id={"sp": dst},
            device_id_type=MESH,
        )

    def one_slot(piece, at):
        slot = piece * per + at
        off = pl.multiple_of(lax.rem(d * hl + slot, heads) * block, block)
        here = pl.ds(off, block)
        xp = jnp.dot(gather, x[:, here], preferred_element_type=jnp.float32)
        before = halo[:, here].astype(jnp.float32)
        taps = cw[:, here].astype(jnp.float32)
        taps = [jnp.broadcast_to(taps[k : k + 1], (SUB, block)) for k in range(CONV)]
        rows = [xp[SUB * j : SUB * (j + 1)] for j in range(steps)]
        early = []
        for m in range(CONV - 1, 0, -1):
            rolled = pltpu.roll(rows[steps - m], 1, 0)
            edge = jnp.broadcast_to(before[SUB - m : SUB - m + 1], (SUB, block))
            early.append(jnp.where(sub == 0, edge, rolled))
        rows = early + rows
        conv = []
        for j in range(steps):
            total = taps[0] * rows[j]
            for k in range(1, CONV):
                total = total + taps[k] * rows[j + k]
            conv.append(total)
        conv = jnp.concatenate(conv, axis=0).astype(jnp.bfloat16)
        pre_r = jnp.dot(conv, w[0, slot], preferred_element_type=jnp.float32)
        pre_i = jnp.dot(conv, w[1, slot], preferred_element_type=jnp.float32)
        pre_r = pre_r.astype(jnp.bfloat16).astype(jnp.float32)
        pre_i = pre_i.astype(jnp.bfloat16).astype(jnp.float32)
        values = conv.astype(jnp.float32)
        factor = softplus_neg(rate[:, here]) * (gate_power / LN2)
        factor = jnp.broadcast_to(factor, (SUB, block))
        h = None
        for j in range(steps):
            part = slice(SUB * j, SUB * (j + 1))
            pace_j = pace_perm[j]
            pace_j = jnp.concatenate([pace_j] * tiles, axis=1)
            r = 1.0 / (1.0 + jnp.exp(-pre_r[part]))
            i = 1.0 / (1.0 + jnp.exp(-pre_i[part]))
            q = pace_j * factor * r
            a = jnp.exp2(-q)
            c = 2.0 * LN2
            series = q * (c + q * (-c * c / 2 + q * (c**3 / 6 - q * (c**4 / 24))))
            gain = jnp.where(q < SMALL, series, 1.0 - a * a)
            b = gain * lax.rsqrt(jnp.maximum(gain, TINY)) * i * values[part]
            if h is None:
                h, total_a = b, a
            else:
                h = a * h + b
                total_a = total_a * a
            hloc[slot, part] = h
            acum[slot, part] = total_a
        for shift in (1, 2, 4):
            inside = sub >= shift
            earlier_a = jnp.where(inside, pltpu.roll(total_a, shift, 0), 1.0)
            earlier_h = jnp.where(inside, pltpu.roll(h, shift, 0), 0.0)
            h = total_a * earlier_h + h
            total_a = total_a * earlier_a
        ex_h[slot] = jnp.where(sub >= 1, pltpu.roll(h, 1, 0), 0.0)
        ex_a[slot] = jnp.where(sub >= 1, pltpu.roll(total_a, 1, 0), 1.0)
        log_a = jnp.log2(jnp.maximum(total_a, TINY))
        for t in range(tiles):
            lanes = slice(LANES * t, LANES * (t + 1))
            stage[pl.ds(at * tiles + t, 1), :] = log_a[SUB - 1 :, lanes]
            stage[pl.ds(SUB + at * tiles + t, 1), :] = h[SUB - 1 :, lanes]

    for piece in range(pieces):
        for o in range(1, ndp):
            if piece * per <= o * hl < (piece + 1) * per:
                w_copies[o - 1].wait_recv()

        @pl.loop(0, per)
        def _(at):
            one_slot(piece, at)

        send_buf[piece] = stage[...].astype(jnp.bfloat16)

        @pl.loop(me + 1, nsp)
        def _(dst):
            carry_copy(piece, me, dst).start()

    def finish_slot(piece, at):
        slot = piece * per + at
        off = pl.multiple_of(lax.rem(d * hl + slot, heads) * block, block)
        start = jnp.concatenate(
            [
                jnp.broadcast_to(carry[pl.ds(at * tiles + t, 1), :], (SUB, LANES))
                for t in range(tiles)
            ],
            axis=1,
        )
        start = ex_h[slot] + ex_a[slot] * start
        states = [
            hloc[slot, SUB * j : SUB * (j + 1)] + acum[slot, SUB * j : SUB * (j + 1)] * start
            for j in range(steps)
        ]
        states = jnp.concatenate(states, axis=0).astype(jnp.bfloat16)
        placed = jnp.dot(scatter, states, preferred_element_type=jnp.float32)
        out_ref[0, :, pl.ds(off, block)] = placed.astype(jnp.bfloat16)

    for piece in range(pieces):
        carry[...] = jnp.zeros_like(carry)

        @pl.loop(0, me)
        def _(src):
            carry_copy(piece, src, me).wait_recv()
            got = recv_buf[src, piece].astype(jnp.float32)
            carry[...] = jnp.exp2(got[:SUB]) * carry[...] + got[SUB:]

        @pl.loop(0, per)
        def _(at):
            finish_slot(piece, at)

    for copy in w_copies:
        copy.wait_send()

    @pl.when(me < nsp - 1)
    def _():
        halo_copy.wait_send()

    for piece in range(pieces):

        @pl.loop(me + 1, nsp)
        def _(dst):
            carry_copy(piece, me, dst).wait_send()


def body(inputs, conv_weight, gate_weight, rate_param, pace):
    nsp = lax.axis_size("sp")
    ndp = lax.axis_size("dp")
    _, count, width = inputs.shape
    block = gate_weight.shape[-1]
    heads = width // block
    pieces = width // PIECE
    f32, bf16 = jnp.float32, jnp.bfloat16
    anywhere = pl.BlockSpec(memory_space=pl.ANY)
    dma = pltpu.SemaphoreType.DMA
    return pl.pallas_call(
        functools.partial(kernel, nsp, ndp, heads, block),
        out_shape=jax.ShapeDtypeStruct(inputs.shape, bf16),
        in_specs=[anywhere] * 5,
        out_specs=pl.BlockSpec(memory_space=pltpu.VMEM),
        scratch_shapes=[
            pltpu.VMEM((count, width), bf16),
            pltpu.VMEM(conv_weight.shape, bf16),
            pltpu.VMEM((2, heads, block, block), bf16),
            pltpu.VMEM((1, width), f32),
            pltpu.VMEM((1, count), f32),
            pltpu.VMEM((count, LANES), f32),
            pltpu.VMEM((count // SUB, SUB, LANES), f32),
            pltpu.VMEM((SUB, width), bf16),
            pltpu.VMEM((heads, count, block), f32),
            pltpu.VMEM((heads, count, block), f32),
            pltpu.VMEM((heads, SUB, block), f32),
            pltpu.VMEM((heads, SUB, block), f32),
            pltpu.VMEM((2 * SUB, LANES), f32),
            pltpu.VMEM((pieces, 2 * SUB, LANES), bf16),
            pltpu.VMEM((nsp, pieces, 2 * SUB, LANES), bf16),
            pltpu.VMEM((SUB, LANES), f32),
            dma((5,)),
            dma((ndp,)),
            dma((ndp,)),
            dma((1,)),
            dma((1,)),
            dma((nsp, pieces)),
            dma((nsp, pieces)),
        ],
        compiler_params=pltpu.CompilerParams(collective_id=0, has_side_effects=True),
    )(inputs, conv_weight, gate_weight, rate_param.reshape(1, width), pace)


def solution(mesh):
    return jax.shard_map(
        body,
        mesh=mesh,
        in_specs=(P("dp", "sp", None), P(), P(None, "dp", None, None), P(), P("dp", None)),
        out_specs=P("dp", "sp", None),
        check_vma=False,
    )
```

```python
import functools
import math

import jax
import jax.numpy as jnp
from jax import lax
from jax.experimental import pallas as pl
from jax.experimental.pallas import tpu as pltpu
from jax.sharding import PartitionSpec as P

CONV = 4
EDGE = CONV - 1
gate_power = 8.0
SUB = 8
LANES = 128
PIECE = SUB * LANES
TINY = 1.2e-38
LN2 = math.log(2.0)
SMALL = 0.07
NEAR = 4
MESH = pl.DeviceIdType.MESH


def softplus_neg(rate):
    e = jnp.exp(-jnp.abs(rate))
    series = e * (1.0 + e * (-0.5 + e * (1.0 / 3.0 + e * (-0.25 + e * 0.2))))
    return jnp.maximum(-rate, 0.0) + jnp.where(e < 0.03, series, jnp.log(1.0 + e))


def kernel(
    nsp, ndp, heads, block,
    x_hbm, cw_hbm, w_hbm, rate_hbm, pace_hbm, out_ref,
    x, cw, w, rate, pace_row, pace_mat, pace_perm, halo,
    ends, hloc, acum, ex_h, ex_a, stage, send_buf, recv_buf, carry,
    known, load_sem, w_send, w_recv, halo_send, halo_recv, c_send, c_recv,
):
    me = lax.axis_index("sp")
    d = lax.axis_index("dp")
    count, width = x.shape
    steps = count // SUB
    hl = heads // ndp
    pieces = width // PIECE
    per = PIECE // block
    tiles = block // LANES

    barrier = pltpu.get_barrier_semaphore()

    def at_distance(delta, ahead, then):
        there = me + delta if ahead else me - delta

        @pl.when(there < nsp if ahead else there >= 0)
        def _():
            then(there)

    def greet(there):
        pl.semaphore_signal(barrier, inc=1, device_id={"sp": there}, device_id_type=MESH)

    near = range(1, min(NEAR, nsp - 1) + 1)
    for delta in near:
        for ahead in (True, False):
            at_distance(delta, ahead, greet)

    @pl.loop(1, ndp)
    def _(o):
        pl.semaphore_signal(barrier, inc=1, device_id={"dp": lax.rem(d + o, ndp)}, device_id_type=MESH)

    first = pl.multiple_of(me * count, count)
    loads = [
        pltpu.make_async_copy(x_hbm.at[0], x, load_sem.at[0]),
        pltpu.make_async_copy(w_hbm, w.at[:, pl.ds(0, hl)], load_sem.at[1]),
        pltpu.make_async_copy(cw_hbm, cw, load_sem.at[2]),
        pltpu.make_async_copy(rate_hbm, rate, load_sem.at[3]),
        pltpu.make_async_copy(pace_hbm.at[:, pl.ds(first, count)], pace_row, load_sem.at[4]),
    ]
    for load in loads:
        load.start()

    @pl.when(me == 0)
    def _():
        halo[...] = jnp.zeros_like(halo)

    rounds = []
    while NEAR * 2 ** len(rounds) < nsp - 1:
        rounds.append(NEAR * 2 ** len(rounds))

    def tell(n):
        for ahead in (True, False):
            at_distance(rounds[n], ahead, lambda there, ahead=ahead: pl.semaphore_signal(
                known.at[n, int(ahead)], inc=1, device_id={"sp": there}, device_id_type=MESH))

    def learn(n):
        for ahead in (True, False):
            at_distance(rounds[n], ahead, lambda _, ahead=ahead: pl.semaphore_wait(
                known.at[n, int(not ahead)], 1))

    w_copies = []
    for slot in range(hl, heads):
        o, own = slot // hl, slot % hl
        w_copies.append(pltpu.make_async_remote_copy(
            src_ref=w.at[:, own],
            dst_ref=w.at[:, slot],
            send_sem=w_send.at[slot],
            recv_sem=w_recv.at[slot],
            device_id={"dp": lax.rem(d - o + ndp, ndp)},
            device_id_type=MESH,
        ))
    halo_copy = pltpu.make_async_remote_copy(
        src_ref=x.at[pl.ds(count - SUB, SUB)],
        dst_ref=halo,
        send_sem=halo_send.at[0],
        recv_sem=halo_recv.at[0],
        device_id={"sp": lax.rem(me + 1, nsp)},
        device_id_type=MESH,
    )
    for load in loads:
        load.wait()

    def meet_and_send():
        reach = len(near)
        peers = jnp.minimum(me, reach) + jnp.minimum(nsp - 1 - me, reach)
        pl.semaphore_wait(barrier, peers + ndp - 1)

        @pl.when(me < nsp - 1)
        def _():
            halo_copy.start()

        for copy in w_copies:
            copy.start()
        if rounds:
            tell(0)

    spread = jnp.broadcast_to(pace_row[...], (LANES, count)).T
    pace_mat[...] = spread
    for j in range(steps):
        pace_perm[j] = pace_mat[pl.ds(j, SUB, stride=steps), :]

    row = lax.broadcasted_iota(jnp.int32, (count, count), 0)
    col = lax.broadcasted_iota(jnp.int32, (count, count), 1)
    gather = jnp.where(col == (row % SUB) * steps + row // SUB, 1.0, 0.0).astype(jnp.bfloat16)
    scatter = jnp.where(row == (col % SUB) * steps + col // SUB, 1.0, 0.0).astype(jnp.bfloat16)
    sub = lax.broadcasted_iota(jnp.int32, (SUB, block), 0)

    def carry_copy(piece, src, dst):
        return pltpu.make_async_remote_copy(
            src_ref=send_buf.at[piece],
            dst_ref=recv_buf.at[src, piece],
            send_sem=c_send.at[dst, piece],
            recv_sem=c_recv.at[src, piece],
            device_id={"sp": dst},
            device_id_type=MESH,
        )

    def take_halo():
        @pl.when(me > 0)
        def _():
            halo_copy.wait_recv()

        if rounds:
            learn(len(rounds) - 1)

    def columns(slot):
        return pl.ds(pl.multiple_of(lax.rem(d * hl + slot, heads) * block, block), block)

    def convolve(rows, here):
        taps = cw[:, here].astype(jnp.float32)
        taps = [jnp.broadcast_to(taps[k : k + 1], (SUB, block)) for k in range(CONV)]
        out = []
        for j in range(len(rows) - EDGE):
            total = taps[0] * rows[j]
            for k in range(1, CONV):
                total = total + taps[k] * rows[j + k]
            out.append(total)
        return out

    def terms(conv, slot, here, first_step):
        conv = jnp.concatenate(conv, axis=0).astype(jnp.bfloat16)
        pre_r = jnp.dot(conv, w[0, slot], preferred_element_type=jnp.float32)
        pre_i = jnp.dot(conv, w[1, slot], preferred_element_type=jnp.float32)
        pre_r = pre_r.astype(jnp.bfloat16).astype(jnp.float32)
        pre_i = pre_i.astype(jnp.bfloat16).astype(jnp.float32)
        values = conv.astype(jnp.float32)
        factor = softplus_neg(rate[:, here]) * (gate_power / LN2)
        factor = jnp.broadcast_to(factor, (SUB, block))
        for j in range(conv.shape[0] // SUB):
            part = slice(SUB * j, SUB * (j + 1))
            pace_j = jnp.concatenate([pace_perm[first_step + j]] * tiles, axis=1)
            r = 1.0 / (1.0 + jnp.exp(-pre_r[part]))
            i = 1.0 / (1.0 + jnp.exp(-pre_i[part]))
            q = pace_j * factor * r
            a = jnp.exp2(-q)
            c = 2.0 * LN2
            series = q * (c + q * (-c * c / 2 + q * (c**3 / 6 - q * (c**4 / 24))))
            gain = jnp.where(q < SMALL, series, 1.0 - a * a)
            b = gain * lax.rsqrt(jnp.maximum(gain, TINY)) * i * values[part]
            yield a, b

    def scan(pairs, slot, first_step):
        h = total_a = None
        for j, (a, b) in enumerate(pairs, first_step):
            if h is None:
                h, total_a = b, a
            else:
                h = a * h + b
                total_a = total_a * a
            part = slice(SUB * j, SUB * (j + 1))
            hloc[slot, part] = h
            acum[slot, part] = total_a

    def main_slot(slot):
        here = columns(slot)
        xp = jnp.dot(gather, x[:, here], preferred_element_type=jnp.float32)
        rows = [xp[SUB * j : SUB * (j + 1)] for j in range(steps)]
        ends[slot] = jnp.concatenate(rows[steps - EDGE :] + rows[:EDGE], axis=0)
        scan(terms(convolve(rows, here), slot, here, EDGE), slot, EDGE)

    def edge_slot(piece, at):
        slot = piece * per + at
        here = columns(slot)
        before = halo[:, here].astype(jnp.float32)
        rows = [ends[slot, SUB * j : SUB * (j + 1)] for j in range(2 * EDGE)]
        for j in range(EDGE):
            edge = before[SUB - EDGE + j : SUB - EDGE + j + 1]
            rows[j] = jnp.where(sub == 0, jnp.broadcast_to(edge, (SUB, block)), pltpu.roll(rows[j], 1, 0))
        conv = convolve(rows, here)
        scan(terms(conv, slot, here, 0), slot, 0)
        edge_end = slice(SUB * (EDGE - 1), SUB * EDGE)
        chunk_end = slice(SUB * (steps - 1), SUB * steps)
        h = hloc[slot, chunk_end] + acum[slot, chunk_end] * hloc[slot, edge_end]
        total_a = acum[slot, chunk_end] * acum[slot, edge_end]
        for shift in (1, 2, 4):
            inside = sub >= shift
            earlier_a = jnp.where(inside, pltpu.roll(total_a, shift, 0), 1.0)
            earlier_h = jnp.where(inside, pltpu.roll(h, shift, 0), 0.0)
            h = total_a * earlier_h + h
            total_a = total_a * earlier_a
        ex_h[slot] = jnp.where(sub >= 1, pltpu.roll(h, 1, 0), 0.0)
        ex_a[slot] = jnp.where(sub >= 1, pltpu.roll(total_a, 1, 0), 1.0)
        log_a = jnp.log2(jnp.maximum(total_a, TINY))
        for t in range(tiles):
            lanes = slice(LANES * t, LANES * (t + 1))
            stage[pl.ds(at * tiles + t, 1), :] = log_a[SUB - 1 :, lanes]
            stage[pl.ds(SUB + at * tiles + t, 1), :] = h[SUB - 1 :, lanes]

    def main_slots(low, high):
        for slot in range(max(hl, low), high):
            w_copies[slot - hl].wait_recv()

        @pl.loop(low, high)
        def _(slot):
            main_slot(slot)

    def edge_and_send(piece):
        @pl.loop(0, per)
        def _(at):
            edge_slot(piece, at)

        send_buf[piece] = stage[...].astype(jnp.bfloat16)

        @pl.loop(me + 1, nsp)
        def _(dst):
            carry_copy(piece, me, dst).start()

    half = per // 2
    for piece in range(pieces):
        low = piece * per
        if piece == 0:
            if hl > half:
                main_slots(low, low + half)
                meet_and_send()
            else:
                main_slots(low, low + hl)
                meet_and_send()
                main_slots(low + hl, low + half)
            main_slots(low + half, low + per)
            for n in range(1, len(rounds)):
                learn(n - 1)
                tell(n)
        else:
            main_slots(low, low + half)
            if piece == 1:
                take_halo()
                edge_and_send(0)
            main_slots(low + half, low + per)
            edge_and_send(piece)

    def finish_slot(piece, at):
        slot = piece * per + at
        off = pl.multiple_of(lax.rem(d * hl + slot, heads) * block, block)
        start = jnp.concatenate(
            [
                jnp.broadcast_to(carry[pl.ds(at * tiles + t, 1), :], (SUB, LANES))
                for t in range(tiles)
            ],
            axis=1,
        )
        start = ex_h[slot] + ex_a[slot] * start
        edge_end = slice(SUB * (EDGE - 1), SUB * EDGE)
        later = hloc[slot, edge_end] + acum[slot, edge_end] * start
        states = [
            hloc[slot, SUB * j : SUB * (j + 1)]
            + acum[slot, SUB * j : SUB * (j + 1)] * (start if j < EDGE else later)
            for j in range(steps)
        ]
        states = jnp.concatenate(states, axis=0).astype(jnp.bfloat16)
        placed = jnp.dot(scatter, states, preferred_element_type=jnp.float32)
        out_ref[0, :, pl.ds(off, block)] = placed.astype(jnp.bfloat16)

    for piece in range(pieces):
        carry[...] = jnp.zeros_like(carry)

        @pl.loop(0, me)
        def _(src):
            carry_copy(piece, src, me).wait_recv()
            got = recv_buf[src, piece].astype(jnp.float32)
            carry[...] = jnp.exp2(got[:SUB]) * carry[...] + got[SUB:]

        @pl.loop(0, per)
        def _(at):
            finish_slot(piece, at)

    for copy in w_copies:
        copy.wait_send()

    @pl.when(me < nsp - 1)
    def _():
        halo_copy.wait_send()

    for piece in range(pieces):

        @pl.loop(me + 1, nsp)
        def _(dst):
            carry_copy(piece, me, dst).wait_send()


def body(inputs, conv_weight, gate_weight, rate_param, pace):
    nsp = lax.axis_size("sp")
    ndp = lax.axis_size("dp")
    _, count, width = inputs.shape
    block = gate_weight.shape[-1]
    heads = width // block
    pieces = width // PIECE
    f32, bf16 = jnp.float32, jnp.bfloat16
    hbm = pl.BlockSpec(memory_space=pltpu.HBM)
    dma = pltpu.SemaphoreType.DMA
    return pl.pallas_call(
        functools.partial(kernel, nsp, ndp, heads, block),
        out_shape=pltpu.VMEM(inputs.shape, bf16),
        in_specs=[hbm] * 5,
        out_specs=pl.BlockSpec(memory_space=pltpu.VMEM),
        scratch_shapes=[
            pltpu.VMEM((count, width), bf16),
            pltpu.VMEM(conv_weight.shape, bf16),
            pltpu.VMEM((2, heads, block, block), bf16),
            pltpu.VMEM((1, width), f32),
            pltpu.VMEM((1, count), f32),
            pltpu.VMEM((count, LANES), f32),
            pltpu.VMEM((count // SUB, SUB, LANES), f32),
            pltpu.VMEM((SUB, width), bf16),
            pltpu.VMEM((heads, 2 * EDGE * SUB, block), f32),
            pltpu.VMEM((heads, count, block), f32),
            pltpu.VMEM((heads, count, block), f32),
            pltpu.VMEM((heads, SUB, block), f32),
            pltpu.VMEM((heads, SUB, block), f32),
            pltpu.VMEM((2 * SUB, LANES), f32),
            pltpu.VMEM((pieces, 2 * SUB, LANES), bf16),
            pltpu.VMEM((nsp, pieces, 2 * SUB, LANES), bf16),
            pltpu.VMEM((SUB, LANES), f32),
            pltpu.SemaphoreType.REGULAR((8, 2)),
            dma((5,)),
            dma((heads,)),
            dma((heads,)),
            dma((1,)),
            dma((1,)),
            dma((nsp, pieces)),
            dma((nsp, pieces)),
        ],
        compiler_params=pltpu.CompilerParams(collective_id=0, has_side_effects=True),
    )(inputs, conv_weight, gate_weight, rate_param.reshape(1, width), pace)


def solution(mesh):
    return jax.shard_map(
        body,
        mesh=mesh,
        in_specs=(P("dp", "sp", None), P(), P(None, "dp", None, None), P(), P("dp", None)),
        out_specs=P("dp", "sp", None),
        check_vma=False,
    )
```

```python
import functools
import math

import jax
import jax.numpy as jnp
from jax import lax
from jax.experimental import pallas as pl
from jax.experimental.pallas import tpu as pltpu
from jax.sharding import PartitionSpec as P

CONV = 4
EDGE = CONV - 1
gate_power = 8.0
SUB = 8
LANES = 128
PIECE = SUB * LANES
TINY = 1.2e-38
LN2 = math.log(2.0)
SMALL = 0.015
SPLIT = 2
NEAR = 4
MESH = pl.DeviceIdType.MESH


def softplus_neg(rate):
    e = jnp.exp(-jnp.abs(rate))
    series = e * (1.0 + e * (-0.5 + e * (1.0 / 3.0 + e * (-0.25 + e * 0.2))))
    return jnp.maximum(-rate, 0.0) + jnp.where(e < 0.03, series, jnp.log(1.0 + e))


def kernel(
    nsp, ndp, heads, block,
    x_hbm, cw_hbm, w_hbm, rate_hbm, pace_hbm, out_ref,
    x, cw, w, rate, pace_row, pace_mat, pace_perm, halo,
    ends, hloc, acum, ex_h, ex_a, stage, send_buf, recv_buf, carry,
    known, load_sem, w_send, w_recv, halo_send, halo_recv, c_send, c_recv,
):
    me = lax.axis_index("sp")
    d = lax.axis_index("dp")
    count, width = x.shape
    steps = count // SUB
    hl = heads // ndp
    pieces = width // PIECE
    per = PIECE // block
    tiles = block // LANES

    barrier = pltpu.get_barrier_semaphore()

    def at_distance(delta, ahead, then):
        there = me + delta if ahead else me - delta

        @pl.when(there < nsp if ahead else there >= 0)
        def _():
            then(there)

    def greet(there):
        pl.semaphore_signal(barrier, inc=1, device_id={"sp": there}, device_id_type=MESH)

    near = range(1, min(NEAR, nsp - 1) + 1)
    for delta in near:
        for ahead in (True, False):
            at_distance(delta, ahead, greet)

    @pl.loop(1, ndp)
    def _(o):
        pl.semaphore_signal(barrier, inc=1, device_id={"dp": lax.rem(d + o, ndp)}, device_id_type=MESH)

    first = pl.multiple_of(me * count, count)
    loads = [
        pltpu.make_async_copy(x_hbm.at[0], x, load_sem.at[0]),
        pltpu.make_async_copy(w_hbm, w.at[:, pl.ds(0, hl)], load_sem.at[1]),
        pltpu.make_async_copy(cw_hbm, cw, load_sem.at[2]),
        pltpu.make_async_copy(rate_hbm, rate, load_sem.at[3]),
        pltpu.make_async_copy(pace_hbm.at[:, pl.ds(first, count)], pace_row, load_sem.at[4]),
    ]
    for load in loads:
        load.start()

    @pl.when(me == 0)
    def _():
        halo[...] = jnp.zeros_like(halo)

    rounds = []
    while NEAR * 2 ** len(rounds) < nsp - 1:
        rounds.append(NEAR * 2 ** len(rounds))

    def tell(n):
        for ahead in (True, False):
            at_distance(rounds[n], ahead, lambda there, ahead=ahead: pl.semaphore_signal(
                known.at[n, int(ahead)], inc=1, device_id={"sp": there}, device_id_type=MESH))

    def learn(n):
        for ahead in (True, False):
            at_distance(rounds[n], ahead, lambda _, ahead=ahead: pl.semaphore_wait(
                known.at[n, int(not ahead)], 1))

    w_copies = []
    for slot in range(hl, heads):
        o, own = slot // hl, slot % hl
        w_copies.append(pltpu.make_async_remote_copy(
            src_ref=w.at[:, own],
            dst_ref=w.at[:, slot],
            send_sem=w_send.at[slot],
            recv_sem=w_recv.at[slot],
            device_id={"dp": lax.rem(d - o + ndp, ndp)},
            device_id_type=MESH,
        ))
    halo_copy = pltpu.make_async_remote_copy(
        src_ref=x.at[pl.ds(count - SUB, SUB)],
        dst_ref=halo,
        send_sem=halo_send.at[0],
        recv_sem=halo_recv.at[0],
        device_id={"sp": lax.rem(me + 1, nsp)},
        device_id_type=MESH,
    )
    for load in loads:
        load.wait()

    def meet_and_send():
        reach = len(near)
        peers = jnp.minimum(me, reach) + jnp.minimum(nsp - 1 - me, reach)
        pl.semaphore_wait(barrier, peers + ndp - 1)

        @pl.when(me < nsp - 1)
        def _():
            halo_copy.start()

        for copy in w_copies:
            copy.start()
        if rounds:
            tell(0)

    spread = jnp.broadcast_to(pace_row[...], (LANES, count)).T
    pace_mat[...] = spread
    for j in range(steps):
        pace_perm[j] = pace_mat[pl.ds(j, SUB, stride=steps), :]

    row = lax.broadcasted_iota(jnp.int32, (count, count), 0)
    col = lax.broadcasted_iota(jnp.int32, (count, count), 1)
    gather = jnp.where(col == (row % SUB) * steps + row // SUB, 1.0, 0.0).astype(jnp.bfloat16)
    scatter = jnp.where(row == (col % SUB) * steps + col // SUB, 1.0, 0.0).astype(jnp.bfloat16)
    sub = lax.broadcasted_iota(jnp.int32, (SUB, block), 0)

    def carry_copy(piece, src, dst):
        return pltpu.make_async_remote_copy(
            src_ref=send_buf.at[piece],
            dst_ref=recv_buf.at[src, piece],
            send_sem=c_send.at[dst, piece],
            recv_sem=c_recv.at[src, piece],
            device_id={"sp": dst},
            device_id_type=MESH,
        )

    def take_halo():
        @pl.when(me > 0)
        def _():
            halo_copy.wait_recv()

    def columns(slot):
        return pl.ds(pl.multiple_of(lax.rem(d * hl + slot, heads) * block, block), block)

    def convolve(rows, here):
        taps = cw[:, here].astype(jnp.float32)
        taps = [jnp.broadcast_to(taps[k : k + 1], (SUB, block)) for k in range(CONV)]
        out = []
        for j in range(len(rows) - EDGE):
            total = taps[0] * rows[j]
            for k in range(1, CONV):
                total = total + taps[k] * rows[j + k]
            out.append(total)
        return out

    def terms(conv, slot, here, first_step):
        conv = jnp.concatenate(conv, axis=0).astype(jnp.bfloat16)
        pre_r = jnp.dot(conv, w[0, slot], preferred_element_type=jnp.float32)
        pre_i = jnp.dot(conv, w[1, slot], preferred_element_type=jnp.float32)
        values = conv.astype(jnp.float32)
        factor = softplus_neg(rate[:, here]) * (gate_power / LN2)
        factor = jnp.broadcast_to(factor, (SUB, block))
        for j in range(conv.shape[0] // SUB):
            part = slice(SUB * j, SUB * (j + 1))
            pace_j = jnp.concatenate([pace_perm[first_step + j]] * tiles, axis=1)
            r = 1.0 / (1.0 + jnp.exp(-pre_r[part]))
            i = 1.0 / (1.0 + jnp.exp(-pre_i[part]))
            q = pace_j * factor * r
            a = jnp.exp2(-q)
            c = 2.0 * LN2
            series = q * (c + q * (c**3 / 6 * q - c * c / 2))
            gain = jnp.where(q < SMALL, series, 1.0 - a * a)
            b = gain * lax.rsqrt(jnp.maximum(gain, TINY)) * i * values[part]
            yield a, b

    def scan(pairs, slot, first_step):
        h = total_a = None
        for j, (a, b) in enumerate(pairs, first_step):
            if h is None:
                h, total_a = b, a
            else:
                h = a * h + b
                total_a = total_a * a
            part = slice(SUB * j, SUB * (j + 1))
            hloc[slot, part] = h
            acum[slot, part] = total_a

    def main_slot(slot):
        here = columns(slot)
        xp = jnp.dot(gather, x[:, here], preferred_element_type=jnp.float32)
        rows = [xp[SUB * j : SUB * (j + 1)] for j in range(steps)]
        ends[slot] = jnp.concatenate(rows[steps - EDGE :] + rows[:EDGE], axis=0)
        scan(terms(convolve(rows, here), slot, here, EDGE), slot, EDGE)

    def with_halo(rows, here):
        before = halo[:, here].astype(jnp.float32)
        out = []
        for j in range(EDGE):
            edge = before[SUB - EDGE + j : SUB - EDGE + j + 1]
            out.append(jnp.where(sub == 0, jnp.broadcast_to(edge, (SUB, block)), pltpu.roll(rows[j], 1, 0)))
        return out

    def full_slot(piece, at):
        slot = piece * per + at
        here = columns(slot)
        xp = jnp.dot(gather, x[:, here], preferred_element_type=jnp.float32)
        rows = [xp[SUB * j : SUB * (j + 1)] for j in range(steps)]
        rows = with_halo(rows[steps - EDGE :], here) + rows
        scan(terms(convolve(rows, here), slot, here, 0), slot, 0)
        chunk_end = slice(SUB * (steps - 1), SUB * steps)
        totals(slot, at, hloc[slot, chunk_end], acum[slot, chunk_end])

    def edge_slot(piece, at):
        slot = piece * per + at
        here = columns(slot)
        rows = [ends[slot, SUB * j : SUB * (j + 1)] for j in range(2 * EDGE)]
        rows = with_halo(rows[:EDGE], here) + rows[EDGE:]
        conv = convolve(rows, here)
        scan(terms(conv, slot, here, 0), slot, 0)
        edge_end = slice(SUB * (EDGE - 1), SUB * EDGE)
        chunk_end = slice(SUB * (steps - 1), SUB * steps)
        h = hloc[slot, chunk_end] + acum[slot, chunk_end] * hloc[slot, edge_end]
        totals(slot, at, h, acum[slot, chunk_end] * acum[slot, edge_end])

    def totals(slot, at, h, total_a):
        for shift in (1, 2, 4):
            inside = sub >= shift
            earlier_a = jnp.where(inside, pltpu.roll(total_a, shift, 0), 1.0)
            earlier_h = jnp.where(inside, pltpu.roll(h, shift, 0), 0.0)
            h = total_a * earlier_h + h
            total_a = total_a * earlier_a
        ex_h[slot] = jnp.where(sub >= 1, pltpu.roll(h, 1, 0), 0.0)
        ex_a[slot] = jnp.where(sub >= 1, pltpu.roll(total_a, 1, 0), 1.0)
        log_a = jnp.log2(jnp.maximum(total_a, TINY))
        for t in range(tiles):
            lanes = slice(LANES * t, LANES * (t + 1))
            stage[pl.ds(at * tiles + t, 1), :] = log_a[SUB - 1 :, lanes]
            stage[pl.ds(SUB + at * tiles + t, 1), :] = h[SUB - 1 :, lanes]

    def wait_maps(low, high):
        for slot in range(max(hl, low), high):
            w_copies[slot - hl].wait_recv()

    def main_slots(low, high):
        wait_maps(low, high)

        @pl.loop(low, high, unroll=True)
        def _(slot):
            main_slot(slot)

    def edge_and_send(piece, split):
        @pl.loop(0, split, unroll=True)
        def _(at):
            edge_slot(piece, at)

        if split < per:
            wait_maps(piece * per + split, piece * per + per)

            @pl.loop(split, per, unroll=True)
            def _(at):
                full_slot(piece, at)

        send_buf[piece] = stage[...].astype(jnp.bfloat16)

        if piece == 0 and rounds:
            learn(len(rounds) - 1)

        @pl.loop(me + 1, nsp)
        def _(dst):
            carry_copy(piece, me, dst).start()

    half = per // 2
    for piece in range(pieces):
        low = piece * per
        if piece == 0:
            if hl > half:
                main_slots(low, low + half)
                meet_and_send()
            else:
                main_slots(low, low + hl)
                meet_and_send()
                main_slots(low + hl, low + half)
            main_slots(low + half, low + per)
            for n in range(1, len(rounds)):
                learn(n - 1)
                tell(n)
        else:
            ahead = SPLIT if piece == 1 else 0
            if ahead:
                main_slots(low, low + ahead)
            if piece == 1:
                take_halo()
                edge_and_send(0, per)
            edge_and_send(piece, ahead)

    def finish_slot(piece, at):
        slot = piece * per + at
        off = pl.multiple_of(lax.rem(d * hl + slot, heads) * block, block)
        start = jnp.concatenate(
            [
                jnp.broadcast_to(carry[pl.ds(at * tiles + t, 1), :], (SUB, LANES))
                for t in range(tiles)
            ],
            axis=1,
        )
        start = ex_h[slot] + ex_a[slot] * start
        edge_end = slice(SUB * (EDGE - 1), SUB * EDGE)
        later = start
        if piece == 0 or at < SPLIT:
            later = hloc[slot, edge_end] + acum[slot, edge_end] * start
        states = [
            hloc[slot, SUB * j : SUB * (j + 1)]
            + acum[slot, SUB * j : SUB * (j + 1)] * (start if j < EDGE else later)
            for j in range(steps)
        ]
        states = jnp.concatenate(states, axis=0).astype(jnp.bfloat16)
        placed = jnp.dot(scatter, states, preferred_element_type=jnp.float32)
        out_ref[0, :, pl.ds(off, block)] = placed.astype(jnp.bfloat16)

    for piece in range(pieces):
        carry[...] = jnp.zeros_like(carry)

        @pl.loop(0, me)
        def _(src):
            carry_copy(piece, src, me).wait_recv()
            got = recv_buf[src, piece].astype(jnp.float32)
            carry[...] = jnp.exp2(got[:SUB]) * carry[...] + got[SUB:]

        for at in range(per):
            finish_slot(piece, at)

    for copy in w_copies:
        copy.wait_send()

    @pl.when(me < nsp - 1)
    def _():
        halo_copy.wait_send()

    for piece in range(pieces):

        @pl.loop(me + 1, nsp)
        def _(dst):
            carry_copy(piece, me, dst).wait_send()


def body(inputs, conv_weight, gate_weight, rate_param, pace):
    nsp = lax.axis_size("sp")
    ndp = lax.axis_size("dp")
    _, count, width = inputs.shape
    block = gate_weight.shape[-1]
    heads = width // block
    pieces = width // PIECE
    f32, bf16 = jnp.float32, jnp.bfloat16
    hbm = pl.BlockSpec(memory_space=pltpu.HBM)
    dma = pltpu.SemaphoreType.DMA
    return pl.pallas_call(
        functools.partial(kernel, nsp, ndp, heads, block),
        out_shape=pltpu.VMEM(inputs.shape, bf16),
        in_specs=[hbm] * 5,
        out_specs=pl.BlockSpec(memory_space=pltpu.VMEM),
        scratch_shapes=[
            pltpu.VMEM((count, width), bf16),
            pltpu.VMEM(conv_weight.shape, bf16),
            pltpu.VMEM((2, heads, block, block), bf16),
            pltpu.VMEM((1, width), f32),
            pltpu.VMEM((1, count), f32),
            pltpu.VMEM((count, LANES), f32),
            pltpu.VMEM((count // SUB, SUB, LANES), f32),
            pltpu.VMEM((SUB, width), bf16),
            pltpu.VMEM((heads, 2 * EDGE * SUB, block), f32),
            pltpu.VMEM((heads, count, block), f32),
            pltpu.VMEM((heads, count, block), f32),
            pltpu.VMEM((heads, SUB, block), f32),
            pltpu.VMEM((heads, SUB, block), f32),
            pltpu.VMEM((2 * SUB, LANES), f32),
            pltpu.VMEM((pieces, 2 * SUB, LANES), bf16),
            pltpu.VMEM((nsp, pieces, 2 * SUB, LANES), bf16),
            pltpu.VMEM((SUB, LANES), f32),
            pltpu.SemaphoreType.REGULAR((8, 2)),
            dma((5,)),
            dma((heads,)),
            dma((heads,)),
            dma((1,)),
            dma((1,)),
            dma((nsp, pieces)),
            dma((nsp, pieces)),
        ],
        compiler_params=pltpu.CompilerParams(collective_id=0, has_side_effects=True),
    )(inputs, conv_weight, gate_weight, rate_param.reshape(1, width), pace)


def solution(mesh):
    return jax.shard_map(
        body,
        mesh=mesh,
        in_specs=(P("dp", "sp", None), P(), P(None, "dp", None, None), P(), P("dp", None)),
        out_specs=P("dp", "sp", None),
        check_vma=False,
    )
```

```python
import functools
import math

import jax
import jax.numpy as jnp
from jax import lax
from jax.experimental import pallas as pl
from jax.experimental.pallas import tpu as pltpu
from jax.sharding import PartitionSpec as P

CONV = 4
EDGE = CONV - 1
gate_power = 8.0
SUB = 8
LANES = 128
PIECE = SUB * LANES
TINY = 1.2e-38
LN2 = math.log(2.0)
SMALL = 0.015
SPLIT = 2
FIRST = 1
NEAR = 4
MESH = pl.DeviceIdType.MESH


def softplus_neg(rate):
    e = jnp.exp(-jnp.abs(rate))
    series = e * (1.0 + e * (-0.5 + e * (1.0 / 3.0 + e * (-0.25 + e * 0.2))))
    return jnp.maximum(-rate, 0.0) + jnp.where(e < 0.03, series, jnp.log(1.0 + e))


def kernel(
    nsp, ndp, heads, block,
    x_hbm, cw_hbm, w_hbm, rate_hbm, pace_hbm, out_ref,
    x, cw, w, rate, pace_row, pace_mat, pace_perm, halo,
    ends, hloc, acum, ex_h, ex_a, stage, send_buf, recv_buf, carry,
    known, load_sem, map_sem, w_send, w_recv, halo_send, halo_recv, c_send, c_recv,
):
    me = lax.axis_index("sp")
    d = lax.axis_index("dp")
    count, width = x.shape
    steps = count // SUB
    hl = heads // ndp
    pieces = width // PIECE
    per = PIECE // block
    tiles = block // LANES

    barrier = pltpu.get_barrier_semaphore()

    def at_distance(delta, ahead, then):
        there = me + delta if ahead else me - delta

        @pl.when(there < nsp if ahead else there >= 0)
        def _():
            then(there)

    def greet(there):
        pl.semaphore_signal(barrier, inc=1, device_id={"sp": there}, device_id_type=MESH)

    near = range(1, min(NEAR, nsp - 1) + 1)
    for delta in near:
        for ahead in (True, False):
            at_distance(delta, ahead, greet)

    @pl.loop(1, ndp)
    def _(o):
        pl.semaphore_signal(barrier, inc=1, device_id={"dp": lax.rem(d + o, ndp)}, device_id_type=MESH)

    first = pl.multiple_of(me * count, count)
    loads = [
        pltpu.make_async_copy(x_hbm.at[0], x, load_sem.at[0]),
        pltpu.make_async_copy(cw_hbm, cw, load_sem.at[1]),
        pltpu.make_async_copy(rate_hbm, rate, load_sem.at[2]),
        pltpu.make_async_copy(pace_hbm.at[:, pl.ds(first, count)], pace_row, load_sem.at[3]),
    ]
    map_loads = [
        pltpu.make_async_copy(w_hbm.at[:, own], w.at[:, own], map_sem.at[own])
        for own in range(hl)
    ]
    for load in loads + map_loads:
        load.start()

    @pl.when(me == 0)
    def _():
        halo[...] = jnp.zeros_like(halo)

    rounds = []
    while NEAR * 2 ** len(rounds) < nsp - 1:
        rounds.append(NEAR * 2 ** len(rounds))

    def tell(n):
        for ahead in (True, False):
            at_distance(rounds[n], ahead, lambda there, ahead=ahead: pl.semaphore_signal(
                known.at[n, int(ahead)], inc=1, device_id={"sp": there}, device_id_type=MESH))

    def learn(n):
        for ahead in (True, False):
            at_distance(rounds[n], ahead, lambda _, ahead=ahead: pl.semaphore_wait(
                known.at[n, int(not ahead)], 1))

    w_copies = []
    for slot in range(hl, heads):
        o, own = slot // hl, slot % hl
        w_copies.append(pltpu.make_async_remote_copy(
            src_ref=w.at[:, own],
            dst_ref=w.at[:, slot],
            send_sem=w_send.at[slot],
            recv_sem=w_recv.at[slot],
            device_id={"dp": lax.rem(d - o + ndp, ndp)},
            device_id_type=MESH,
        ))
    halo_copy = pltpu.make_async_remote_copy(
        src_ref=x.at[pl.ds(count - SUB, SUB)],
        dst_ref=halo,
        send_sem=halo_send.at[0],
        recv_sem=halo_recv.at[0],
        device_id={"sp": lax.rem(me + 1, nsp)},
        device_id_type=MESH,
    )
    for load in loads:
        load.wait()

    def meet_and_send():
        reach = len(near)
        peers = jnp.minimum(me, reach) + jnp.minimum(nsp - 1 - me, reach)
        pl.semaphore_wait(barrier, peers + ndp - 1)

        @pl.when(me < nsp - 1)
        def _():
            halo_copy.start()

        for copy in w_copies:
            copy.start()
        if rounds:
            tell(0)

    spread = jnp.broadcast_to(pace_row[...], (LANES, count)).T
    pace_mat[...] = spread
    for j in range(steps):
        pace_perm[j] = pace_mat[pl.ds(j, SUB, stride=steps), :]

    row = lax.broadcasted_iota(jnp.int32, (count, count), 0)
    col = lax.broadcasted_iota(jnp.int32, (count, count), 1)
    gather = jnp.where(col == (row % SUB) * steps + row // SUB, 1.0, 0.0).astype(jnp.bfloat16)
    scatter = jnp.where(row == (col % SUB) * steps + col // SUB, 1.0, 0.0).astype(jnp.bfloat16)
    sub = lax.broadcasted_iota(jnp.int32, (SUB, block), 0)

    def carry_copy(piece, src, dst):
        return pltpu.make_async_remote_copy(
            src_ref=send_buf.at[piece],
            dst_ref=recv_buf.at[src, piece],
            send_sem=c_send.at[dst, piece],
            recv_sem=c_recv.at[src, piece],
            device_id={"sp": dst},
            device_id_type=MESH,
        )

    def take_halo():
        @pl.when(me > 0)
        def _():
            halo_copy.wait_recv()

    def columns(slot):
        return pl.ds(pl.multiple_of(lax.rem(d * hl + slot, heads) * block, block), block)

    def convolve(rows, here):
        taps = cw[:, here].astype(jnp.float32)
        taps = [jnp.broadcast_to(taps[k : k + 1], (SUB, block)) for k in range(CONV)]
        out = []
        for j in range(len(rows) - EDGE):
            total = taps[0] * rows[j]
            for k in range(1, CONV):
                total = total + taps[k] * rows[j + k]
            out.append(total)
        return out

    def terms(conv, slot, here, first_step):
        conv = jnp.concatenate(conv, axis=0).astype(jnp.bfloat16)
        pre_r = jnp.dot(conv, w[0, slot], preferred_element_type=jnp.float32)
        pre_i = jnp.dot(conv, w[1, slot], preferred_element_type=jnp.float32)
        values = conv.astype(jnp.float32)
        factor = softplus_neg(rate[:, here]) * (gate_power / LN2)
        factor = jnp.broadcast_to(factor, (SUB, block))
        for j in range(conv.shape[0] // SUB):
            part = slice(SUB * j, SUB * (j + 1))
            pace_j = jnp.concatenate([pace_perm[first_step + j]] * tiles, axis=1)
            r = 1.0 / (1.0 + jnp.exp(-pre_r[part]))
            i = 1.0 / (1.0 + jnp.exp(-pre_i[part]))
            q = pace_j * factor * r
            a = jnp.exp2(-q)
            c = 2.0 * LN2
            series = q * (c + q * (c**3 / 6 * q - c * c / 2))
            gain = jnp.where(q < SMALL, series, 1.0 - a * a)
            b = gain * lax.rsqrt(jnp.maximum(gain, TINY)) * i * values[part]
            yield a, b

    def scan(pairs, slot, first_step):
        h = total_a = None
        for j, (a, b) in enumerate(pairs, first_step):
            if h is None:
                h, total_a = b, a
            else:
                h = a * h + b
                total_a = total_a * a
            part = slice(SUB * j, SUB * (j + 1))
            hloc[slot, part] = h
            acum[slot, part] = total_a

    def main_slot(slot):
        here = columns(slot)
        xp = jnp.dot(gather, x[:, here], preferred_element_type=jnp.float32)
        rows = [xp[SUB * j : SUB * (j + 1)] for j in range(steps)]
        ends[slot] = jnp.concatenate(rows[steps - EDGE :] + rows[:EDGE], axis=0)
        scan(terms(convolve(rows, here), slot, here, EDGE), slot, EDGE)

    def with_halo(rows, here):
        before = halo[:, here].astype(jnp.float32)
        out = []
        for j in range(EDGE):
            edge = before[SUB - EDGE + j : SUB - EDGE + j + 1]
            out.append(jnp.where(sub == 0, jnp.broadcast_to(edge, (SUB, block)), pltpu.roll(rows[j], 1, 0)))
        return out

    def full_slot(piece, at):
        slot = piece * per + at
        here = columns(slot)
        xp = jnp.dot(gather, x[:, here], preferred_element_type=jnp.float32)
        rows = [xp[SUB * j : SUB * (j + 1)] for j in range(steps)]
        rows = with_halo(rows[steps - EDGE :], here) + rows
        scan(terms(convolve(rows, here), slot, here, 0), slot, 0)
        chunk_end = slice(SUB * (steps - 1), SUB * steps)
        totals(slot, at, hloc[slot, chunk_end], acum[slot, chunk_end])

    def edge_slot(piece, at):
        slot = piece * per + at
        here = columns(slot)
        rows = [ends[slot, SUB * j : SUB * (j + 1)] for j in range(2 * EDGE)]
        rows = with_halo(rows[:EDGE], here) + rows[EDGE:]
        conv = convolve(rows, here)
        scan(terms(conv, slot, here, 0), slot, 0)
        edge_end = slice(SUB * (EDGE - 1), SUB * EDGE)
        chunk_end = slice(SUB * (steps - 1), SUB * steps)
        h = hloc[slot, chunk_end] + acum[slot, chunk_end] * hloc[slot, edge_end]
        totals(slot, at, h, acum[slot, chunk_end] * acum[slot, edge_end])

    def totals(slot, at, h, total_a):
        for shift in (1, 2, 4):
            inside = sub >= shift
            earlier_a = jnp.where(inside, pltpu.roll(total_a, shift, 0), 1.0)
            earlier_h = jnp.where(inside, pltpu.roll(h, shift, 0), 0.0)
            h = total_a * earlier_h + h
            total_a = total_a * earlier_a
        ex_h[slot] = jnp.where(sub >= 1, pltpu.roll(h, 1, 0), 0.0)
        ex_a[slot] = jnp.where(sub >= 1, pltpu.roll(total_a, 1, 0), 1.0)
        log_a = jnp.log2(jnp.maximum(total_a, TINY))
        for t in range(tiles):
            lanes = slice(LANES * t, LANES * (t + 1))
            stage[pl.ds(at * tiles + t, 1), :] = log_a[SUB - 1 :, lanes]
            stage[pl.ds(SUB + at * tiles + t, 1), :] = h[SUB - 1 :, lanes]

    def wait_maps(low, high):
        for slot in range(max(hl, low), high):
            w_copies[slot - hl].wait_recv()

    def main_slots(low, high):
        wait_maps(low, high)

        @pl.loop(low, high, unroll=True)
        def _(slot):
            main_slot(slot)

    def edge_and_send(piece, split):
        @pl.loop(0, split, unroll=True)
        def _(at):
            edge_slot(piece, at)

        if split < per:
            wait_maps(piece * per + split, piece * per + per)

            @pl.loop(split, per, unroll=True)
            def _(at):
                full_slot(piece, at)

        send_buf[piece] = stage[...].astype(jnp.bfloat16)

        if piece == 0 and rounds:
            learn(len(rounds) - 1)

        @pl.loop(me + 1, nsp)
        def _(dst):
            carry_copy(piece, me, dst).start()

    half = per // 2
    for piece in range(pieces):
        low = piece * per
        if piece == 0:
            begun = low + min(hl, FIRST)
            for load in map_loads[:begun]:
                load.wait()
            middle = begun + (low + per - begun) // 2
            main_slots(low, begun)
            for load in map_loads[begun:]:
                load.wait()
            meet_and_send()
            main_slots(begun, middle)
            for n in range(1, len(rounds)):
                learn(n - 1)
                tell(n)
            main_slots(middle, low + per)
        else:
            ahead = SPLIT if piece == 1 else 0
            if ahead:
                main_slots(low, low + ahead)
            if piece == 1:
                take_halo()
                edge_and_send(0, per)
            edge_and_send(piece, ahead)

    def finish_slot(piece, at):
        slot = piece * per + at
        off = pl.multiple_of(lax.rem(d * hl + slot, heads) * block, block)
        start = jnp.concatenate(
            [
                jnp.broadcast_to(carry[pl.ds(at * tiles + t, 1), :], (SUB, LANES))
                for t in range(tiles)
            ],
            axis=1,
        )
        start = ex_h[slot] + ex_a[slot] * start
        edge_end = slice(SUB * (EDGE - 1), SUB * EDGE)
        later = start
        if piece == 0 or at < SPLIT:
            later = hloc[slot, edge_end] + acum[slot, edge_end] * start
        states = [
            hloc[slot, SUB * j : SUB * (j + 1)]
            + acum[slot, SUB * j : SUB * (j + 1)] * (start if j < EDGE else later)
            for j in range(steps)
        ]
        states = jnp.concatenate(states, axis=0).astype(jnp.bfloat16)
        placed = jnp.dot(scatter, states, preferred_element_type=jnp.float32)
        out_ref[0, :, pl.ds(off, block)] = placed.astype(jnp.bfloat16)

    for piece in range(pieces):
        carry[...] = jnp.zeros_like(carry)

        @pl.loop(0, me)
        def _(src):
            carry_copy(piece, src, me).wait_recv()
            got = recv_buf[src, piece].astype(jnp.float32)
            carry[...] = jnp.exp2(got[:SUB]) * carry[...] + got[SUB:]

        for at in range(per):
            finish_slot(piece, at)

    for copy in w_copies:
        copy.wait_send()

    @pl.when(me < nsp - 1)
    def _():
        halo_copy.wait_send()

    for piece in range(pieces):

        @pl.loop(me + 1, nsp)
        def _(dst):
            carry_copy(piece, me, dst).wait_send()


def body(inputs, conv_weight, gate_weight, rate_param, pace):
    nsp = lax.axis_size("sp")
    ndp = lax.axis_size("dp")
    _, count, width = inputs.shape
    block = gate_weight.shape[-1]
    heads = width // block
    hl = heads // ndp
    pieces = width // PIECE
    f32, bf16 = jnp.float32, jnp.bfloat16
    hbm = pl.BlockSpec(memory_space=pltpu.HBM)
    dma = pltpu.SemaphoreType.DMA
    return pl.pallas_call(
        functools.partial(kernel, nsp, ndp, heads, block),
        out_shape=pltpu.VMEM(inputs.shape, bf16),
        in_specs=[hbm] * 5,
        out_specs=pl.BlockSpec(memory_space=pltpu.VMEM),
        scratch_shapes=[
            pltpu.VMEM((count, width), bf16),
            pltpu.VMEM(conv_weight.shape, bf16),
            pltpu.VMEM((2, heads, block, block), bf16),
            pltpu.VMEM((1, width), f32),
            pltpu.VMEM((1, count), f32),
            pltpu.VMEM((count, LANES), f32),
            pltpu.VMEM((count // SUB, SUB, LANES), f32),
            pltpu.VMEM((SUB, width), bf16),
            pltpu.VMEM((heads, 2 * EDGE * SUB, block), f32),
            pltpu.VMEM((heads, count, block), f32),
            pltpu.VMEM((heads, count, block), f32),
            pltpu.VMEM((heads, SUB, block), f32),
            pltpu.VMEM((heads, SUB, block), f32),
            pltpu.VMEM((2 * SUB, LANES), f32),
            pltpu.VMEM((pieces, 2 * SUB, LANES), bf16),
            pltpu.VMEM((nsp, pieces, 2 * SUB, LANES), bf16),
            pltpu.VMEM((SUB, LANES), f32),
            pltpu.SemaphoreType.REGULAR((8, 2)),
            dma((4,)),
            dma((hl,)),
            dma((heads,)),
            dma((heads,)),
            dma((1,)),
            dma((1,)),
            dma((nsp, pieces)),
            dma((nsp, pieces)),
        ],
        compiler_params=pltpu.CompilerParams(collective_id=0, has_side_effects=True),
    )(inputs, conv_weight, gate_weight, rate_param.reshape(1, width), pace)


def solution(mesh):
    return jax.shard_map(
        body,
        mesh=mesh,
        in_specs=(P("dp", "sp", None), P(), P(None, "dp", None, None), P(), P("dp", None)),
        out_specs=P("dp", "sp", None),
        check_vma=False,
    )
```
